32 devices in a mesh: grp: 2 (over x), ep: 8 (over z, y), tp: 2 (over core).
Axes of the slice: x: 2, y: 2, z: 4, core: 2. Of those that a mesh axis runs over, the one named last changes fastest.
Arguments:
- tokens: bfloat16 [2048, 4096], P(('grp', 'ep')), parts along dimension 0, may hold values from -16 to 16, as said below
- norm_gain: float32 [4096], replicated, may hold values from 0.1 to 1.9
- gate_weight: bfloat16 [8, 4096, 768], P('ep', None, 'tp'), may hold values from -0.09375 to 0.09375
- up_weight: bfloat16 [8, 4096, 768], P('ep', None, 'tp'), may hold values from -0.09375 to 0.09375
- down_weight: bfloat16 [8, 768, 4096], P('ep', 'tp'), may hold values from -0.21875 to 0.21875
- chosen: int32 [16, 8, 20], P(('grp', 'ep')), parts along dimension 0, may hold values from 0 to 128, as said below
- affinity: float32 [16, 8, 20], P(('grp', 'ep')), parts along dimension 0, may hold values from 0.2 to 1
Outputs:
- mixed: bfloat16 [2048, 4096], P(('grp', 'ep'), 'tp'), parts along dimension 0
The draws below stay inside these ranges and needn't reach their ends.
There are 2 independent parts, one for each index of `grp`. The reference program is written for one: setup_inputs(seed, part) draws one part's arguments, and reference() takes and returns one part's arrays. A program takes and returns all parts, laid end to end along the dimension named above; an argument that names none is the same for every part. Nothing has to cross between parts.
Inputs may be any that keep to these rules, and one draw needn't show every extreme that they name: `tokens`: draws differ in their scale from row to row. `chosen`: in each (block, expert) row the live entries come first and are distinct; dead entries equal 128. Every expert has exactly 128 live slots in all and at least one live slot in every block; some block gives some expert exactly 20 live slots.
All inputs are finite; a program needn't handle non-finite values.
Results may differ from the reference program's by a relative error of at most 0.0095.
Values may be sent and summed in bfloat16 or wider, within the bound.
A program may use at most 64 MiB of HBM per device.

```python
import math
import jax
import jax.numpy as jnp
from jax import lax

D = 4096
FF = 768
TOK_DEV = 128
TOKENS = 1024
EXPERTS = 8
SLOT = 20
N_EP = 8
N_TP = 2


def draw_tokens(key, part):
    first_key, second_key = jax.random.split(key)
    base = jnp.clip(jax.random.normal(first_key, (TOKENS, D), jnp.float32), -4.0, 4.0)
    row_scale = jnp.exp(jax.random.uniform(second_key, (TOKENS, 1), jnp.float32, math.log(0.3), math.log(3.0)))
    return (base * row_scale).astype(jnp.bfloat16)


def draw_chosen(key, part):
    half_axis = N_EP // 2
    average = TOK_DEV // 8
    spread = SLOT - average
    keys = jax.random.split(key, 4)
    delta = jax.random.randint(keys[0], (EXPERTS, half_axis), 0, spread + 1)
    forced = jax.random.randint(keys[1], (EXPERTS, 1), 0, half_axis)
    delta = jnp.where(jnp.arange(half_axis)[None, :] == forced, spread, delta)
    signs = jax.random.randint(keys[2], (EXPERTS, half_axis), 0, 2) * 2 - 1
    counts = jnp.concatenate([average + signs * delta, average - signs * delta], axis=1)
    per_block = jnp.transpose(counts)
    scores = jax.random.randint(keys[3], (N_EP, EXPERTS, TOK_DEV), 0, 1 << 20) * TOK_DEV + jnp.arange(TOK_DEV)[None, None, :]
    order = jnp.argsort(scores, axis=-1, stable=True)[:, :, :SLOT]
    picks = jnp.where(jnp.arange(SLOT)[None, None, :] < per_block[:, :, None], order, TOK_DEV)
    return picks.astype(jnp.int32)


def steps_of(own_key, extent, pieces, smallest, high):
    factor_of = 1.0
    for position, blocks in pieces:
        heights = jax.random.uniform(jax.random.fold_in(jax.random.fold_in(own_key, 6), position), (blocks,), jnp.float32, smallest / len(pieces), high / len(pieces))
        factor_of = factor_of * jnp.repeat(jnp.exp(heights), extent[position] // blocks).reshape((-1,) + (1,) * (len(extent) - 1 - position))
    return factor_of


def normal_values(key, shape, scale, reach, pieces=(), kind=jnp.bfloat16):
    values = scale * jax.random.normal(key, shape, jnp.float32)
    if pieces:
        values = values * steps_of(key, shape, pieces, -0.22, 0.18)
    return jnp.clip(values, -reach, reach).astype(kind)


def setup_inputs(seed: int = 0, part: int = 0) -> dict:
    seeds = jax.random.split(jax.random.key(seed), 8)
    part_splits = jax.random.split(jax.random.fold_in(seeds[7], part), 8)
    return {
        "tokens": draw_tokens(jax.random.fold_in(jax.random.fold_in(seeds[7], part), 71), part),
        "norm_gain": jnp.clip(1.0 + 0.18 * jax.random.normal(seeds[1], (D,), jnp.float32), 0.1, 1.9),
        "gate_weight": normal_values(seeds[2], (EXPERTS, D, FF), D ** -0.5, 0.09375, ((0, 8), (2, 2))),
        "up_weight": normal_values(seeds[3], (EXPERTS, D, FF), D ** -0.5, 0.09375, ((0, 8), (2, 2))),
        "down_weight": normal_values(seeds[4], (EXPERTS, FF, D), FF ** -0.5, 0.21875, ((0, 8), (1, 2))),
        "chosen": draw_chosen(jax.random.fold_in(jax.random.fold_in(seeds[7], part), 71), part),
        "affinity": jnp.clip(0.2 + 0.8 * jax.random.uniform(part_splits[6], (N_EP, EXPERTS, SLOT), jnp.float32) ** steps_of(part_splits[6], (N_EP, EXPERTS, SLOT), ((0, 8),), -0.2, 0.2), 0.2, 1.0),
    }


norm_eps = 1e-06

def normalize(block, norm_gain):
    values = block.astype(jnp.float32)
    scaled = values * lax.rsqrt(lax.optimization_barrier(jnp.mean(values * values, axis=-1, keepdims=True)) + norm_eps)
    return (scaled * norm_gain.astype(jnp.float32)).astype(jnp.bfloat16)

def reference(tokens, norm_gain, gate_weight, up_weight, down_weight, chosen, affinity):
    total_rows = tokens.shape[0]
    model_width = tokens.shape[1]
    normed = normalize(tokens, norm_gain)
    ff_block = FF // N_TP
    block_base = jnp.arange(N_EP, dtype=jnp.int32)[:, None] * TOK_DEV

    def expert_step(carry, index):
        picks = chosen[:, index, :]
        live = picks < TOK_DEV
        global_rows = (block_base + jnp.minimum(picks, TOK_DEV - 1)).reshape(-1).astype(jnp.int32)
        picked = normed[global_rows]
        gate_proj = jnp.dot(picked, gate_weight[index], preferred_element_type=jnp.float32)
        up_value = jnp.dot(picked, up_weight[index], preferred_element_type=jnp.float32)
        hidden = (jax.nn.silu(gate_proj) * up_value).astype(jnp.bfloat16)
        partial_sum = jnp.zeros((picked.shape[0], model_width), jnp.float32)
        for piece_index in range(N_TP):
            lower = piece_index * ff_block
            piece = jnp.dot(hidden[:, lower:lower + ff_block], down_weight[index, lower:lower + ff_block], preferred_element_type=jnp.float32)
            partial_sum = partial_sum + piece.astype(jnp.bfloat16).astype(jnp.float32)
        expert_out = partial_sum.astype(jnp.bfloat16)
        weight = jnp.where(live, affinity[:, index, :], 0.0).astype(jnp.bfloat16).reshape(-1)
        contrib = weight.astype(jnp.float32)[:, None] * expert_out.astype(jnp.float32)
        target = jnp.where(live.reshape(-1), global_rows, total_rows).astype(jnp.int32)
        return (carry.at[target].add(contrib, mode='drop'), None)
    start_sum = jnp.zeros((total_rows, model_width), jnp.float32)
    result, unused = lax.scan(expert_step, start_sum, jnp.arange(chosen.shape[1], dtype=jnp.int32))
    return result.astype(jnp.bfloat16)
```

```python
import functools

import jax
import jax.numpy as jnp
from jax import lax
from jax.experimental import pallas as pl
from jax.experimental.pallas import tpu as pltpu
from jax.sharding import PartitionSpec as P

norm_eps = 1e-06
CHUNKS = 4
bf16, f32 = jnp.bfloat16, jnp.float32


def dot(a, b):
    return jnp.dot(a, b, preferred_element_type=f32)


def iota(shape, dim):
    return lax.broadcasted_iota(jnp.int32, shape, dim)


def kernel(n, pad, tok_hbm, gain_ref, gate_hbm, up_hbm, down_hbm, chosen_ref, aff_ref, out_ref,
           tok, gate_w, up_w, down_own, down_other, picks, arrived, hid_own, hid_other, outs, ret, acc,
           load_sem, wd_sem, pick_send, pick_recv, relay_send, relay_recv, hid_sem, ret_send, ret_recv):
    me = lax.axis_index("ep")
    h = lax.axis_index("tp")
    partner = 1 - h
    rows, width = tok.shape
    half = width // 2
    cc = half // CHUNKS
    slot = chosen_ref.shape[1]
    total = n * pad
    offsets = sorted(range(1, n), key=lambda o: (-min(o, n - o), o))

    load_tok = pltpu.make_async_copy(tok_hbm, tok, load_sem.at[0])
    load_tok.start()

    barrier = pltpu.get_barrier_semaphore()
    for o in range(1, n):
        pl.semaphore_signal(barrier, inc=1, device_id={"ep": lax.rem(me + o, n)}, device_id_type=pl.DeviceIdType.MESH)
    pl.semaphore_signal(barrier, inc=1, device_id={"tp": partner}, device_id_type=pl.DeviceIdType.MESH)

    my_cols = pl.multiple_of(h * half, half)
    partner_cols = pl.multiple_of(partner * half, half)
    load_gate = pltpu.make_async_copy(gate_hbm.at[0], gate_w, load_sem.at[1])
    load_up = pltpu.make_async_copy(up_hbm.at[0], up_w, load_sem.at[2])
    load_down = pltpu.make_async_copy(down_hbm.at[0, :, pl.ds(my_cols, half)], down_own, load_sem.at[3])
    load_gate.start()
    load_up.start()
    load_down.start()

    picked = chosen_ref[...].astype(f32)
    owner = iota((total, n), 0)
    first = iota((total, n), 1) * pad
    spread = jnp.where((owner >= first) & (owner < first + pad), 1.0, 0.0).astype(bf16)
    wide = dot(spread, picked.astype(bf16))
    within = lax.rem(iota((total, slot), 0), pad) == iota((total, slot), 1)
    column = jnp.sum(jnp.where(within, wide + 1.0, 0.0), axis=1, keepdims=True) - 1.0
    select = jnp.where(iota((total, rows), 1).astype(f32) == column, 1.0, 0.0).astype(bf16)

    load_tok.wait()
    squares = jnp.zeros((rows, 1), f32)
    for i in range(8):
        piece = tok[:, i * (width // 8):(i + 1) * (width // 8)].astype(f32)
        squares = squares + jnp.sum(piece * piece, axis=1, keepdims=True)
    scale = lax.rsqrt(squares / width + norm_eps)

    pl.semaphore_wait(barrier, n)

    def pick_copy(c, dest, src):
        return pltpu.make_async_remote_copy(
            picks.at[c, dest], arrived.at[0, c, src], pick_send.at[c, dest], pick_recv.at[c, src],
            device_id={"ep": dest}, device_id_type=pl.DeviceIdType.MESH)

    def relay_copy(c, src, source):
        return pltpu.make_async_remote_copy(
            source, arrived.at[1, c, src], relay_send.at[c, src], relay_recv.at[c, src],
            device_id={"tp": partner}, device_id_type=pl.DeviceIdType.MESH)

    for c in range(CHUNKS):
        cols = pl.ds(pl.multiple_of(h * half + c * cc, cc), cc)
        normed = (tok[:, cols].astype(f32) * scale * gain_ref[:, cols]).astype(bf16)
        picks[c] = dot(select, normed).astype(bf16).reshape(n, pad, cc)
        for o in offsets:
            dest = lax.rem(me + o, n)
            pick_copy(c, dest, me).start()
        arrived[0, c, pl.ds(me, 1)] = picks[c, pl.ds(me, 1)]
        relay_copy(c, me, picks.at[c, me]).start()

    send_down = pltpu.make_async_remote_copy(
        down_hbm.at[0, :, pl.ds(partner_cols, half)], down_other, wd_sem.at[0], wd_sem.at[1],
        device_id={"tp": partner}, device_id_type=pl.DeviceIdType.MESH)
    send_down.start()

    place = jnp.where(lax.rem(iota((slot, total), 1), pad) == iota((slot, total), 0), 1.0, 0.0).astype(bf16)
    lane = iota((n, total), 1)
    low = iota((n, total), 0) * pad
    mine = (lane >= low) & (lane < low + pad)
    pick_row = jnp.sum(jnp.where(mine, dot(picked.astype(bf16), place), 0.0), axis=0, keepdims=True)
    filled = lax.rem(iota((1, total), 1), pad) < slot
    pick_row = jnp.where(filled, pick_row, -1.0)
    aff_row = jnp.sum(jnp.where(mine, dot(aff_ref[...].astype(bf16), place), 0.0), axis=0, keepdims=True)
    combine = jnp.where(iota((rows, total), 0).astype(f32) == pick_row, aff_row, 0.0).astype(bf16)

    load_gate.wait()
    load_up.wait()
    for c in range(CHUNKS):
        for o in offsets:
            src = lax.rem(me + n - o, n)
            pick_copy(c, src, src).wait_recv()
            relay_copy(c, src, arrived.at[0, c, src]).start()
        for side in range(2):
            if side == 1:
                relay_copy(c, me, picks.at[c, me]).wait_recv()
                for o in offsets:
                    src = lax.rem(me + n - o, n)
                    relay_copy(c, src, arrived.at[0, c, src]).wait_recv()
            base = h if side == 0 else partner
            depth = pl.ds(pl.multiple_of(base * half + c * cc, cc), cc)
            x = arrived[side, c].reshape(total, cc)
            g = dot(x, gate_w[depth, :])
            u = dot(x, up_w[depth, :])
            if c == 0 and side == 0:
                acc[0] = g
                acc[1] = u
            else:
                acc[0] += g
                acc[1] += u
    g = acc[0]
    hid_own[...] = (g / (1.0 + jnp.exp(-g)) * acc[1]).astype(bf16)
    send_hid = pltpu.make_async_remote_copy(
        hid_own, hid_other, hid_sem.at[0], hid_sem.at[1],
        device_id={"tp": partner}, device_id_type=pl.DeviceIdType.MESH)
    send_hid.start()

    def ret_copy(c, dest, src):
        return pltpu.make_async_remote_copy(
            outs.at[c, dest], ret.at[c, src], ret_send.at[c, dest], ret_recv.at[c, src],
            device_id={"ep": dest}, device_id_type=pl.DeviceIdType.MESH)

    load_down.wait()
    for c in range(CHUNKS):
        part = dot(hid_own[...], down_own[:, c * cc:(c + 1) * cc])
        if c == 0:
            send_down.wait_recv()
            send_hid.wait_recv()
        part = part + dot(hid_other[...], down_other[:, c * cc:(c + 1) * cc])
        outs[c] = part.astype(bf16).reshape(n, pad, cc)
        for o in offsets:
            ret_copy(c, lax.rem(me + o, n), me).start()
        ret[c, pl.ds(me, 1)] = outs[c, pl.ds(me, 1)]

    for c in range(CHUNKS):
        for o in offsets:
            src = lax.rem(me + n - o, n)
            ret_copy(c, src, src).wait_recv()
        out_ref[:, c * cc:(c + 1) * cc] = dot(combine, ret[c].reshape(total, cc)).astype(bf16)

    send_down.wait_send()
    send_hid.wait_send()
    for c in range(CHUNKS):
        relay_copy(c, me, picks.at[c, me]).wait_send()
        for o in offsets:
            src = lax.rem(me + n - o, n)
            relay_copy(c, src, arrived.at[0, c, src]).wait_send()
            dest = lax.rem(me + o, n)
            pick_copy(c, dest, me).wait_send()
            ret_copy(c, dest, me).wait_send()


def solution(mesh):
    n = mesh.shape["ep"]

    def shards(tokens, norm_gain, gate_weight, up_weight, down_weight, chosen, affinity):
        rows, width = tokens.shape
        ff = gate_weight.shape[2]
        slot = chosen.shape[2]
        pad = -(-slot // 8) * 8
        half = width // 2
        cc = half // CHUNKS
        any_spec = pl.BlockSpec(memory_space=pl.ANY)
        vmem = pl.BlockSpec(memory_space=pltpu.VMEM)
        dma = pltpu.SemaphoreType.DMA
        return pl.pallas_call(
            functools.partial(kernel, n, pad),
            out_shape=jax.ShapeDtypeStruct((rows, half), bf16),
            in_specs=[any_spec, vmem, any_spec, any_spec, any_spec, vmem, vmem],
            out_specs=vmem,
            scratch_shapes=[
                pltpu.VMEM((rows, width), bf16),
                pltpu.VMEM((width, ff), bf16),
                pltpu.VMEM((width, ff), bf16),
                pltpu.VMEM((ff, half), bf16),
                pltpu.VMEM((ff, half), bf16),
                pltpu.VMEM((CHUNKS, n, pad, cc), bf16),
                pltpu.VMEM((2, CHUNKS, n, pad, cc), bf16),
                pltpu.VMEM((n * pad, ff), bf16),
                pltpu.VMEM((n * pad, ff), bf16),
                pltpu.VMEM((CHUNKS, n, pad, cc), bf16),
                pltpu.VMEM((CHUNKS, n, pad, cc), bf16),
                pltpu.VMEM((2, n * pad, ff), f32),
                dma((4,)),
                dma((2,)),
                dma((CHUNKS, n)),
                dma((CHUNKS, n)),
                dma((CHUNKS, n)),
                dma((CHUNKS, n)),
                dma((2,)),
                dma((CHUNKS, n)),
                dma((CHUNKS, n)),
            ],
            compiler_params=pltpu.CompilerParams(
                collective_id=0, has_side_effects=True, vmem_limit_bytes=56 * 1024 * 1024
            ),
        )(tokens, norm_gain.reshape(1, -1), gate_weight, up_weight, down_weight, chosen[0], affinity[0])

    in_specs = (
        P(("grp", "ep"), None),
        P(),
        P("ep", None, "tp"),
        P("ep", None, "tp"),
        P("ep", "tp", None),
        P(("grp", "ep"), None, None),
        P(("grp", "ep"), None, None),
    )
    out_specs = P(("grp", "ep"), "tp")
    return jax.shard_map(shards, mesh=mesh, in_specs=in_specs, out_specs=out_specs, check_vma=False)
```

```python
import functools

import jax
import jax.numpy as jnp
from jax import lax
from jax.experimental import pallas as pl
from jax.experimental.pallas import tpu as pltpu
from jax.sharding import PartitionSpec as P

norm_eps = 1e-06
bf16, f32 = jnp.bfloat16, jnp.float32


def dot(a, b):
    return jnp.dot(a, b, preferred_element_type=f32)


def iota(shape, dim):
    return lax.broadcasted_iota(jnp.int32, shape, dim)


def merge(y0, y1, full):
    return jnp.concatenate(
        [y0[:, :full] + y1[:, 8:], y0[:, full:] + pltpu.roll(y1[:, :8], 4, 1)], axis=1)


def pack(y, full):
    side = y.shape[2] // 2
    y0, y1 = y[:, :, :side], y[:, :, side:]
    upper = iota((y.shape[0], 8, side), 1) < 4
    rest = jnp.where(upper, y0[:, full:], pltpu.roll(y1[:, full:], 4, 1))
    return jnp.concatenate([y0[:, :full], rest, y1[:, :full]], axis=1).astype(bf16)


def kernel(n, full, tok_hbm, gain_ref, gate_hbm, up_hbm, down_hbm, chosen_ref, aff_ref, out_ref,
           tok, gu_w, down_own, down_other, normed, picks, arrived, hid_own, hid_other, outs, ret,
           load_sem, wd_sem, pick_send, pick_recv, relay_send, relay_recv, hid_send, hid_recv, ret_send, ret_recv):
    me = lax.axis_index("ep")
    h = lax.axis_index("tp")
    partner = 1 - h
    rows, width = tok.shape
    half = width // 2
    side = half // 2
    ff = down_own.shape[0]
    slot = chosen_ref.shape[1]
    pad = full + 8
    total = n * pad
    paired = n & (n - 1) == 0
    mesh_id = pl.DeviceIdType.MESH

    def to(k):
        return me ^ k if paired else lax.rem(me + k, n)

    def back(k):
        return me ^ k if paired else lax.rem(me + n - k, n)

    place_k = (lambda e: e ^ me) if paired else (lambda e: lax.rem(e + n - me, n))
    if n >= 4:
        batches = [(n // 2, n // 2 + n // 4), (0, n // 2), (n // 2 + n // 4, n)]
        order = list(range(n // 2, n)) + list(range(1, n // 2))
    else:
        batches = [(0, n)]
        order = list(range(1, n))

    load_tok = pltpu.make_async_copy(tok_hbm, tok, load_sem.at[0])
    load_tok.start()

    barrier = pltpu.get_barrier_semaphore()
    for k in order:
        pl.semaphore_signal(barrier, inc=1, device_id={"ep": to(k)}, device_id_type=mesh_id)
    pl.semaphore_signal(barrier, inc=1, device_id={"tp": partner}, device_id_type=mesh_id)

    my_cols = pl.multiple_of(h * half, half)
    partner_cols = pl.multiple_of(partner * half, half)
    load_gate = pltpu.make_async_copy(gate_hbm.at[0], gu_w.at[:, :ff], load_sem.at[1])
    load_up = pltpu.make_async_copy(up_hbm.at[0], gu_w.at[:, ff:], load_sem.at[2])
    load_down = pltpu.make_async_copy(down_hbm.at[0, :, pl.ds(my_cols, half)], down_own, load_sem.at[3])
    load_gate.start()
    load_up.start()
    load_down.start()

    picked = chosen_ref[...].astype(f32).astype(bf16)
    row = iota((total, n), 0)
    first = place_k(iota((total, n), 1)) * pad
    spread = jnp.where((row >= first) & (row < first + pad), 1.0, 0.0).astype(bf16)
    wide = dot(spread, picked)
    within = lax.rem(iota((total, slot), 0), pad) == iota((total, slot), 1)
    column = jnp.sum(jnp.where(within, wide + 1.0, 0.0), axis=1, keepdims=True) - 1.0
    select = jnp.where(iota((total, rows), 1).astype(f32) == column, 1.0, 0.0).astype(bf16)

    load_tok.wait()
    squares = jnp.zeros((rows, 1), f32)
    for i in range(8):
        piece = tok[:, i * (width // 8):(i + 1) * (width // 8)].astype(f32)
        squares = squares + jnp.sum(piece * piece, axis=1, keepdims=True)
    scale = lax.rsqrt(squares / width + norm_eps)
    for i in range(4):
        cols = pl.ds(pl.multiple_of(h * half + i * (half // 4), half // 4), half // 4)
        normed[:, i * (half // 4):(i + 1) * (half // 4)] = (
            tok[:, cols].astype(f32) * scale * gain_ref[:, cols]).astype(bf16)

    def pick_copy(k):
        return pltpu.make_async_remote_copy(
            picks.at[k], arrived.at[0, k], pick_send.at[k], pick_recv.at[k],
            device_id={"ep": to(k)}, device_id_type=mesh_id)

    def relay_copy(k):
        source = picks.at[0] if k == 0 else arrived.at[0, k]
        return pltpu.make_async_remote_copy(
            source, arrived.at[1, k], relay_send.at[k], relay_recv.at[k],
            device_id={"tp": partner}, device_id_type=mesh_id)

    def hid_copy(i):
        span = pl.ds(batches[i][0] * pad, (batches[i][1] - batches[i][0]) * pad)
        return pltpu.make_async_remote_copy(
            hid_own.at[span], hid_other.at[span], hid_send.at[i], hid_recv.at[i],
            device_id={"tp": partner}, device_id_type=mesh_id)

    def ret_copy(k):
        return pltpu.make_async_remote_copy(
            outs.at[k], ret.at[k], ret_send.at[k], ret_recv.at[k],
            device_id={"ep": back(k)}, device_id_type=mesh_id)

    for i, (lo, hi) in enumerate(sorted(batches, key=lambda b: b[0] == 0)):
        taken = dot(select[lo * pad:hi * pad], normed[...])
        picks[lo:hi] = pack(taken.reshape(hi - lo, pad, half), full)
        if i == 0:
            pl.semaphore_wait(barrier, n)
        for k in range(max(lo, 1), hi):
            pick_copy(k).start()
    arrived[0, 0] = picks[0]
    relay_copy(0).start()

    send_down = pltpu.make_async_remote_copy(
        down_hbm.at[0, :, pl.ds(partner_cols, half)], down_other, wd_sem.at[0], wd_sem.at[1],
        device_id={"tp": partner}, device_id_type=mesh_id)
    send_down.start()

    slot_low = place_k(iota((n, total), 0)) * pad
    lane = iota((n, total), 1)
    mine = (lane >= slot_low) & (lane < slot_low + pad)
    weights = aff_ref[...].astype(bf16)

    def combine_of(second):
        at = lax.rem(iota((slot, total), 1), pad)
        if second:
            at = jnp.where(at < 4, -1, jnp.where(at < 8, at + (full - 4), at - 8))
        place = jnp.where(at == iota((slot, total), 0), 1.0, 0.0).astype(bf16)
        row_of = jnp.sum(jnp.where(mine, dot(picked, place), 0.0), axis=0, keepdims=True)
        filled = jnp.sum(place.astype(f32), axis=0, keepdims=True)
        row_of = jnp.where(filled > 0.5, row_of, -1.0)
        value = jnp.sum(jnp.where(mine, dot(weights, place), 0.0), axis=0, keepdims=True)
        return jnp.where(iota((rows, total), 0).astype(f32) == row_of, value, 0.0).astype(bf16)

    combine = [combine_of(False), combine_of(True)]

    load_gate.wait()
    load_up.wait()
    for i, (lo, hi) in enumerate(batches):
        count = hi - lo
        for k in range(max(lo, 1), hi):
            pick_copy(k).wait_recv()
            relay_copy(k).start()
        y0, y1 = None, None
        for s, base in ((0, h), (1, partner)):
            if s == 1:
                for k in range(lo, hi):
                    relay_copy(k).wait_recv()
            x0 = arrived[s, lo:hi, :pad].reshape(count * pad, side)
            x1 = arrived[s, lo:hi, full:].reshape(count * pad, side)
            p0 = dot(x0, gu_w[pl.ds(pl.multiple_of(base * half, side), side), :])
            p1 = dot(x1, gu_w[pl.ds(pl.multiple_of(base * half + side, side), side), :])
            y0, y1 = (p0, p1) if s == 0 else (y0 + p0, y1 + p1)
        y = merge(y0.reshape(count, pad, 2 * ff), y1.reshape(count, pad, 2 * ff), full).reshape(count * pad, 2 * ff)
        g = y[:, :ff]
        span = slice(lo * pad, hi * pad)
        hid_own[span] = (g / (1.0 + jnp.exp(-g)) * y[:, ff:]).astype(bf16)
        hid_copy(i).start()
        if i == 0:
            load_down.wait()
        part = dot(hid_own[span], down_own[...])
        if i == 0:
            send_down.wait_recv()
        hid_copy(i).wait_recv()
        part = part + dot(hid_other[span], down_other[...])
        outs[lo:hi] = pack(part.reshape(count, pad, half), full)
        for k in range(max(lo, 1), hi):
            ret_copy(k).start()
        if lo == 0:
            ret[0] = outs[0]

    for i, (lo, hi) in enumerate(batches):
        for k in range(max(lo, 1), hi):
            ret_copy(k).wait_recv()
    out_ref[:, :side] = dot(combine[0], ret[:, :pad].reshape(total, side)).astype(bf16)
    out_ref[:, side:] = dot(combine[1], ret[:, full:].reshape(total, side)).astype(bf16)

    send_down.wait_send()
    for i in range(len(batches)):
        hid_copy(i).wait_send()
    for k in range(n):
        relay_copy(k).wait_send()
        if k:
            pick_copy(k).wait_send()
            ret_copy(k).wait_send()


def solution(mesh):
    n = mesh.shape["ep"]

    def shards(tokens, norm_gain, gate_weight, up_weight, down_weight, chosen, affinity):
        rows, width = tokens.shape
        ff = gate_weight.shape[2]
        slot = chosen.shape[2]
        full = slot // 8 * 8 if 0 < slot % 8 <= 4 else -(-slot // 8) * 8
        pad = full + 8
        half = width // 2
        message = (n, 2 * full + 8, half // 2)
        any_spec = pl.BlockSpec(memory_space=pl.ANY)
        vmem = pl.BlockSpec(memory_space=pltpu.VMEM)
        dma = pltpu.SemaphoreType.DMA
        return pl.pallas_call(
            functools.partial(kernel, n, full),
            out_shape=jax.ShapeDtypeStruct((rows, half), bf16),
            in_specs=[any_spec, vmem, any_spec, any_spec, any_spec, vmem, vmem],
            out_specs=vmem,
            scratch_shapes=[
                pltpu.VMEM((rows, width), bf16),
                pltpu.VMEM((width, 2 * ff), bf16),
                pltpu.VMEM((ff, half), bf16),
                pltpu.VMEM((ff, half), bf16),
                pltpu.VMEM((rows, half), bf16),
                pltpu.VMEM(message, bf16),
                pltpu.VMEM((2,) + message, bf16),
                pltpu.VMEM((n * pad, ff), bf16),
                pltpu.VMEM((n * pad, ff), bf16),
                pltpu.VMEM(message, bf16),
                pltpu.VMEM(message, bf16),
                dma((4,)),
                dma((2,)),
                dma((n,)),
                dma((n,)),
                dma((n,)),
                dma((n,)),
                dma((3,)),
                dma((3,)),
                dma((n,)),
                dma((n,)),
            ],
            compiler_params=pltpu.CompilerParams(
                collective_id=0, has_side_effects=True, vmem_limit_bytes=56 * 1024 * 1024
            ),
        )(tokens, norm_gain.reshape(1, -1), gate_weight, up_weight, down_weight, chosen[0], affinity[0])

    in_specs = (
        P(("grp", "ep"), None),
        P(),
        P("ep", None, "tp"),
        P("ep", None, "tp"),
        P("ep", "tp", None),
        P(("grp", "ep"), None, None),
        P(("grp", "ep"), None, None),
    )
    out_specs = P(("grp", "ep"), "tp")
    return jax.shard_map(shards, mesh=mesh, in_specs=in_specs, out_specs=out_specs, check_vma=False)
```

```python
import functools

import jax
import jax.numpy as jnp
from jax import lax
from jax.experimental import pallas as pl
from jax.experimental.pallas import tpu as pltpu
from jax.sharding import PartitionSpec as P

norm_eps = 1e-06
bf16, f32 = jnp.bfloat16, jnp.float32


def dot(a, b):
    return jnp.dot(a, b, preferred_element_type=f32)


def iota(shape, dim):
    return lax.broadcasted_iota(jnp.int32, shape, dim)


def merge(y0, y1, full):
    return jnp.concatenate(
        [y0[:, :full] + y1[:, 8:], y0[:, full:] + pltpu.roll(y1[:, :8], 4, 1)], axis=1)


def pack(y, full):
    side = y.shape[2] // 2
    y0, y1 = y[:, :, :side], y[:, :, side:]
    upper = iota((y.shape[0], 8, side), 1) < 4
    rest = jnp.where(upper, y0[:, full:], pltpu.roll(y1[:, full:], 4, 1))
    return jnp.concatenate([y0[:, :full], rest, y1[:, :full]], axis=1).astype(bf16)


def kernel(n, full, tok_hbm, gain_hbm, gate_hbm, up_hbm, down_hbm, chosen_hbm, aff_hbm, out_ref,
           tok, gain_ref, chosen_ref, aff_ref, gu_w, down_own, down_other, normed, picks, arrived, hid_own, hid_other, outs, ret,
           load_sem, wd_sem, pick_send, pick_recv, relay_send, relay_recv, hid_send, hid_recv, ret_send, ret_recv):
    me = lax.axis_index("ep")
    h = lax.axis_index("tp")
    partner = 1 - h
    rows, width = tok.shape
    half = width // 2
    side = half // 2
    ff = down_own.shape[0]
    slot = chosen_ref.shape[1]
    pad = full + 8
    total = n * pad
    paired = n & (n - 1) == 0
    mesh_id = pl.DeviceIdType.MESH

    def to(k):
        return me ^ k if paired else lax.rem(me + k, n)

    def back(k):
        return me ^ k if paired else lax.rem(me + n - k, n)

    place_k = (lambda e: e ^ me) if paired else (lambda e: lax.rem(e + n - me, n))
    if n >= 4:
        batches = [(0, n // 2), (n // 2, n // 2 + n // 4), (n // 2 + n // 4, n)]
        order = list(range(n // 2, n)) + list(range(1, n // 2))
    else:
        batches = [(0, n)]
        order = list(range(1, n))

    load_tok = pltpu.make_async_copy(tok_hbm, tok, load_sem.at[0])
    load_tok.start()
    load_gain = pltpu.make_async_copy(gain_hbm, gain_ref, load_sem.at[4])
    load_gain.start()
    load_chosen = pltpu.make_async_copy(chosen_hbm, chosen_ref, load_sem.at[5])
    load_chosen.start()
    load_aff = pltpu.make_async_copy(aff_hbm, aff_ref, load_sem.at[6])
    load_aff.start()

    barrier = pltpu.get_barrier_semaphore()
    for k in order:
        pl.semaphore_signal(barrier, inc=1, device_id={"ep": to(k)}, device_id_type=mesh_id)
    pl.semaphore_signal(barrier, inc=1, device_id={"tp": partner}, device_id_type=mesh_id)

    my_cols = pl.multiple_of(h * half, half)
    partner_cols = pl.multiple_of(partner * half, half)
    load_gate = pltpu.make_async_copy(gate_hbm.at[0], gu_w.at[:, :ff], load_sem.at[1])
    load_up = pltpu.make_async_copy(up_hbm.at[0], gu_w.at[:, ff:], load_sem.at[2])
    load_down = pltpu.make_async_copy(down_hbm.at[0, :, pl.ds(my_cols, half)], down_own, load_sem.at[3])
    load_gate.start()
    load_up.start()
    load_down.start()

    load_chosen.wait()
    picked = chosen_ref[...].astype(f32).astype(bf16)
    row = iota((total, n), 0)
    first = place_k(iota((total, n), 1)) * pad
    spread = jnp.where((row >= first) & (row < first + pad), 1.0, 0.0).astype(bf16)
    wide = dot(spread, picked)
    within = lax.rem(iota((total, slot), 0), pad) == iota((total, slot), 1)
    column = jnp.sum(jnp.where(within, wide + 1.0, 0.0), axis=1, keepdims=True) - 1.0
    select = jnp.where(iota((total, rows), 1).astype(f32) == column, 1.0, 0.0).astype(bf16)

    load_tok.wait()
    load_gain.wait()
    squares = jnp.zeros((rows, 1), f32)
    for i in range(8):
        piece = tok[:, i * (width // 8):(i + 1) * (width // 8)].astype(f32)
        squares = squares + jnp.sum(piece * piece, axis=1, keepdims=True)
    scale = lax.rsqrt(squares / width + norm_eps)
    for i in range(4):
        cols = pl.ds(pl.multiple_of(h * half + i * (half // 4), half // 4), half // 4)
        normed[:, i * (half // 4):(i + 1) * (half // 4)] = (
            tok[:, cols].astype(f32) * scale * gain_ref[:, cols]).astype(bf16)

    def pick_copy(k):
        return pltpu.make_async_remote_copy(
            picks.at[k], arrived.at[0, k], pick_send.at[k], pick_recv.at[k],
            device_id={"ep": to(k)}, device_id_type=mesh_id)

    def relay_copy(k):
        source = picks.at[0] if k == 0 else arrived.at[0, k]
        return pltpu.make_async_remote_copy(
            source, arrived.at[1, k], relay_send.at[k], relay_recv.at[k],
            device_id={"tp": partner}, device_id_type=mesh_id)

    def hid_copy(i):
        span = pl.ds(batches[i][0] * pad, (batches[i][1] - batches[i][0]) * pad)
        return pltpu.make_async_remote_copy(
            hid_own.at[span], hid_other.at[span], hid_send.at[i], hid_recv.at[i],
            device_id={"tp": partner}, device_id_type=mesh_id)

    def ret_copy(k):
        return pltpu.make_async_remote_copy(
            outs.at[k], ret.at[k], ret_send.at[k], ret_recv.at[k],
            device_id={"ep": back(k)}, device_id_type=mesh_id)

    for i, (lo, hi) in enumerate([(0, n // 2), (n // 2, n // 2 + n // 4), (n // 2 + n // 4, n)]):
        taken = dot(select[lo * pad:hi * pad], normed[...])
        picks[lo:hi] = pack(taken.reshape(hi - lo, pad, half), full)
        if i == 0:
            pl.semaphore_wait(barrier, n)
        for k in range(max(lo, 1), hi):
            pick_copy(k).start()
    arrived[0, 0] = picks[0]
    relay_copy(0).start()

    send_down = pltpu.make_async_remote_copy(
        down_hbm.at[0, :, pl.ds(partner_cols, half)], down_other, wd_sem.at[0], wd_sem.at[1],
        device_id={"tp": partner}, device_id_type=mesh_id)
    send_down.start()

    slot_low = place_k(iota((n, total), 0)) * pad
    lane = iota((n, total), 1)
    mine = (lane >= slot_low) & (lane < slot_low + pad)
    load_aff.wait()
    weights = aff_ref[...].astype(bf16)

    def combine_of(second):
        at = lax.rem(iota((slot, total), 1), pad)
        if second:
            at = jnp.where(at < 4, -1, jnp.where(at < 8, at + (full - 4), at - 8))
        place = jnp.where(at == iota((slot, total), 0), 1.0, 0.0).astype(bf16)
        row_of = jnp.sum(jnp.where(mine, dot(picked, place), 0.0), axis=0, keepdims=True)
        filled = jnp.sum(place.astype(f32), axis=0, keepdims=True)
        row_of = jnp.where(filled > 0.5, row_of, -1.0)
        value = jnp.sum(jnp.where(mine, dot(weights, place), 0.0), axis=0, keepdims=True)
        return jnp.where(iota((rows, total), 0).astype(f32) == row_of, value, 0.0).astype(bf16)

    combine = [combine_of(False), combine_of(True)]

    load_gate.wait()
    load_up.wait()
    for i, (lo, hi) in enumerate(batches):
        count = hi - lo
        for k in range(max(lo, 1), hi):
            pick_copy(k).wait_recv()
            relay_copy(k).start()
        y0, y1 = None, None
        for s, base in ((0, h), (1, partner)):
            if s == 1:
                for k in range(lo, hi):
                    relay_copy(k).wait_recv()
            x0 = arrived[s, lo:hi, :pad].reshape(count * pad, side)
            x1 = arrived[s, lo:hi, full:].reshape(count * pad, side)
            p0 = dot(x0, gu_w[pl.ds(pl.multiple_of(base * half, side), side), :])
            p1 = dot(x1, gu_w[pl.ds(pl.multiple_of(base * half + side, side), side), :])
            y0, y1 = (p0, p1) if s == 0 else (y0 + p0, y1 + p1)
        y = merge(y0.reshape(count, pad, 2 * ff), y1.reshape(count, pad, 2 * ff), full).reshape(count * pad, 2 * ff)
        g = y[:, :ff]
        span = slice(lo * pad, hi * pad)
        hid_own[span] = (g / (1.0 + jnp.exp(-g)) * y[:, ff:]).astype(bf16)
        hid_copy(i).start()
        if i == 0:
            load_down.wait()
        part = dot(hid_own[span], down_own[...])
        if i == 0:
            send_down.wait_recv()
        hid_copy(i).wait_recv()
        part = part + dot(hid_other[span], down_other[...])
        outs[lo:hi] = pack(part.reshape(count, pad, half), full)
        for k in range(max(lo, 1), hi):
            ret_copy(k).start()
        if lo == 0:
            ret[0] = outs[0]

    for i, (lo, hi) in enumerate(batches):
        for k in range(max(lo, 1), hi):
            ret_copy(k).wait_recv()
    out_ref[:, :side] = dot(combine[0], ret[:, :pad].reshape(total, side)).astype(bf16)
    out_ref[:, side:] = dot(combine[1], ret[:, full:].reshape(total, side)).astype(bf16)

    send_down.wait_send()
    for i in range(len(batches)):
        hid_copy(i).wait_send()
    for k in range(n):
        relay_copy(k).wait_send()
        if k:
            pick_copy(k).wait_send()
            ret_copy(k).wait_send()


def solution(mesh):
    n = mesh.shape["ep"]

    def shards(tokens, norm_gain, gate_weight, up_weight, down_weight, chosen, affinity):
        rows, width = tokens.shape
        ff = gate_weight.shape[2]
        slot = chosen.shape[2]
        full = slot // 8 * 8 if 0 < slot % 8 <= 4 else -(-slot // 8) * 8
        pad = full + 8
        half = width // 2
        message = (n, 2 * full + 8, half // 2)
        any_spec = pl.BlockSpec(memory_space=pl.ANY)
        vmem = pl.BlockSpec(memory_space=pltpu.VMEM)
        dma = pltpu.SemaphoreType.DMA
        return pl.pallas_call(
            functools.partial(kernel, n, full),
            out_shape=jax.ShapeDtypeStruct((rows, half), bf16),
            in_specs=[any_spec] * 7,
            out_specs=vmem,
            scratch_shapes=[
                pltpu.VMEM((rows, width), bf16),
                pltpu.VMEM((1, width), f32),
                pltpu.VMEM(chosen.shape[1:], jnp.int32),
                pltpu.VMEM(affinity.shape[1:], f32),
                pltpu.VMEM((width, 2 * ff), bf16),
                pltpu.VMEM((ff, half), bf16),
                pltpu.VMEM((ff, half), bf16),
                pltpu.VMEM((rows, half), bf16),
                pltpu.VMEM(message, bf16),
                pltpu.VMEM((2,) + message, bf16),
                pltpu.VMEM((n * pad, ff), bf16),
                pltpu.VMEM((n * pad, ff), bf16),
                pltpu.VMEM(message, bf16),
                pltpu.VMEM(message, bf16),
                dma((7,)),
                dma((2,)),
                dma((n,)),
                dma((n,)),
                dma((n,)),
                dma((n,)),
                dma((3,)),
                dma((3,)),
                dma((n,)),
                dma((n,)),
            ],
            compiler_params=pltpu.CompilerParams(
                collective_id=0, has_side_effects=True, vmem_limit_bytes=56 * 1024 * 1024
            ),
        )(tokens, norm_gain.reshape(1, -1), gate_weight, up_weight, down_weight, chosen[0], affinity[0])

    in_specs = (
        P(("grp", "ep"), None),
        P(),
        P("ep", None, "tp"),
        P("ep", None, "tp"),
        P("ep", "tp", None),
        P(("grp", "ep"), None, None),
        P(("grp", "ep"), None, None),
    )
    out_specs = P(("grp", "ep"), "tp")
    return jax.shard_map(shards, mesh=mesh, in_specs=in_specs, out_specs=out_specs, check_vma=False)
```

```python
import functools

import jax
import jax.numpy as jnp
from jax import lax
from jax.experimental import pallas as pl
from jax.experimental.pallas import tpu as pltpu
from jax.sharding import PartitionSpec as P

norm_eps = 1e-06
bf16, f32 = jnp.bfloat16, jnp.float32


def dot(a, b):
    return jnp.dot(a, b, preferred_element_type=f32)


def iota(shape, dim):
    return lax.broadcasted_iota(jnp.int32, shape, dim)


def merge(y0, y1, full):
    return jnp.concatenate(
        [y0[:, :full] + y1[:, 8:], y0[:, full:] + pltpu.roll(y1[:, :8], 4, 1)], axis=1)


def pack(y, full):
    side = y.shape[2] // 2
    y0, y1 = y[:, :, :side], y[:, :, side:]
    upper = iota((y.shape[0], 8, side), 1) < 4
    rest = jnp.where(upper, y0[:, full:], pltpu.roll(y1[:, full:], 4, 1))
    return jnp.concatenate([y0[:, :full], rest, y1[:, :full]], axis=1).astype(bf16)


def kernel(n, full, tok_hbm, gain_hbm, gate_hbm, up_hbm, down_hbm, chosen_hbm, aff_hbm, ret, factors_hbm,
           factors, tok, gain_ref, chosen_ref, aff_ref, gu_w, down_own, down_other, normed, picks, arrived, hid_own, hid_other, outs,
           load_sem, wd_sem, pick_send, pick_recv, relay_send, relay_recv, hid_send, hid_recv, ret_send, ret_recv):
    me = lax.axis_index("ep")
    h = lax.axis_index("tp")
    partner = 1 - h
    rows, width = tok.shape
    half = width // 2
    side = half // 2
    ff = down_own.shape[0]
    slot = chosen_ref.shape[1]
    pad = full + 8
    total = n * pad
    paired = n & (n - 1) == 0
    mesh_id = pl.DeviceIdType.MESH

    def to(k):
        return me ^ k if paired else lax.rem(me + k, n)

    def back(k):
        return me ^ k if paired else lax.rem(me + n - k, n)

    place_k = (lambda e: e ^ me) if paired else (lambda e: lax.rem(e + n - me, n))
    if n >= 4:
        batches = [(0, n // 2), (n // 2, n // 2 + n // 4), (n // 2 + n // 4, n)]
        order = list(range(n // 2, n)) + list(range(1, n // 2))
    else:
        batches = [(0, n)]
        order = list(range(1, n))

    load_tok = pltpu.make_async_copy(tok_hbm, tok, load_sem.at[0])
    load_tok.start()
    load_gain = pltpu.make_async_copy(gain_hbm, gain_ref, load_sem.at[4])
    load_gain.start()
    load_chosen = pltpu.make_async_copy(chosen_hbm, chosen_ref, load_sem.at[5])
    load_chosen.start()
    load_aff = pltpu.make_async_copy(aff_hbm, aff_ref, load_sem.at[6])
    load_aff.start()

    barrier = pltpu.get_barrier_semaphore()
    for k in order:
        pl.semaphore_signal(barrier, inc=1, device_id={"ep": to(k)}, device_id_type=mesh_id)
    pl.semaphore_signal(barrier, inc=1, device_id={"tp": partner}, device_id_type=mesh_id)

    my_cols = pl.multiple_of(h * half, half)
    partner_cols = pl.multiple_of(partner * half, half)
    load_gate = pltpu.make_async_copy(gate_hbm.at[0], gu_w.at[:, :ff], load_sem.at[1])
    load_up = pltpu.make_async_copy(up_hbm.at[0], gu_w.at[:, ff:], load_sem.at[2])
    load_down = pltpu.make_async_copy(down_hbm.at[0, :, pl.ds(my_cols, half)], down_own, load_sem.at[3])
    load_gate.start()
    load_up.start()
    load_down.start()

    load_chosen.wait()
    picked = chosen_ref[...].astype(f32).astype(bf16)
    row = iota((total, n), 0)
    first = place_k(iota((total, n), 1)) * pad
    spread = jnp.where((row >= first) & (row < first + pad), 1.0, 0.0).astype(bf16)
    wide = dot(spread, picked)
    within = lax.rem(iota((total, slot), 0), pad) == iota((total, slot), 1)
    column = jnp.sum(jnp.where(within, wide + 1.0, 0.0), axis=1, keepdims=True) - 1.0
    select = jnp.where(iota((total, rows), 1).astype(f32) == column, 1.0, 0.0).astype(bf16)

    load_tok.wait()
    load_gain.wait()
    squares = jnp.zeros((rows, 1), f32)
    for i in range(8):
        piece = tok[:, i * (width // 8):(i + 1) * (width // 8)].astype(f32)
        squares = squares + jnp.sum(piece * piece, axis=1, keepdims=True)
    scale = lax.rsqrt(squares / width + norm_eps)
    for i in range(4):
        cols = pl.ds(pl.multiple_of(h * half + i * (half // 4), half // 4), half // 4)
        normed[:, i * (half // 4):(i + 1) * (half // 4)] = (
            tok[:, cols].astype(f32) * scale * gain_ref[:, cols]).astype(bf16)

    def pick_copy(k):
        return pltpu.make_async_remote_copy(
            picks.at[k], arrived.at[0, k], pick_send.at[k], pick_recv.at[k],
            device_id={"ep": to(k)}, device_id_type=mesh_id)

    def relay_copy(k):
        source = picks.at[0] if k == 0 else arrived.at[0, k]
        return pltpu.make_async_remote_copy(
            source, arrived.at[1, k], relay_send.at[k], relay_recv.at[k],
            device_id={"tp": partner}, device_id_type=mesh_id)

    def hid_copy(i):
        span = pl.ds(batches[i][0] * pad, (batches[i][1] - batches[i][0]) * pad)
        return pltpu.make_async_remote_copy(
            hid_own.at[span], hid_other.at[span], hid_send.at[i], hid_recv.at[i],
            device_id={"tp": partner}, device_id_type=mesh_id)

    def ret_copy(k):
        return pltpu.make_async_remote_copy(
            outs.at[k], ret.at[k], ret_send.at[k], ret_recv.at[k],
            device_id={"ep": back(k)}, device_id_type=mesh_id)

    for i, (lo, hi) in enumerate([(0, n // 2), (n // 2, n // 2 + n // 4), (n // 2 + n // 4, n)]):
        taken = dot(select[lo * pad:hi * pad], normed[...])
        picks[lo:hi] = pack(taken.reshape(hi - lo, pad, half), full)
        if i == 0:
            pl.semaphore_wait(barrier, n)
        for k in (range(1, hi) if lo == 0 else range(hi - 1, lo - 1, -1)):
            pick_copy(k).start()
    arrived[0, 0] = picks[0]
    relay_copy(0).start()

    send_down = pltpu.make_async_remote_copy(
        down_hbm.at[0, :, pl.ds(partner_cols, half)], down_other, wd_sem.at[0], wd_sem.at[1],
        device_id={"tp": partner}, device_id_type=mesh_id)
    send_down.start()

    slot_low = place_k(iota((n, total), 0)) * pad
    lane = iota((n, total), 1)
    mine = (lane >= slot_low) & (lane < slot_low + pad)
    load_aff.wait()
    weights = aff_ref[...].astype(bf16)

    def combine_of(second):
        at = lax.rem(iota((slot, total), 1), pad)
        if second:
            at = jnp.where(at < 4, -1, jnp.where(at < 8, at + (full - 4), at - 8))
        place = jnp.where(at == iota((slot, total), 0), 1.0, 0.0).astype(bf16)
        row_of = jnp.sum(jnp.where(mine, dot(picked, place), 0.0), axis=0, keepdims=True)
        filled = jnp.sum(place.astype(f32), axis=0, keepdims=True)
        row_of = jnp.where(filled > 0.5, row_of, -1.0)
        value = jnp.sum(jnp.where(mine, dot(weights, place), 0.0), axis=0, keepdims=True)
        return jnp.where(iota((rows, total), 0).astype(f32) == row_of, value, 0.0).astype(bf16)

    factors[0] = combine_of(False)
    factors[1] = combine_of(True)
    put = pltpu.make_async_copy(factors, factors_hbm, load_sem.at[8])
    put.start()

    load_gate.wait()
    load_up.wait()
    for i, (lo, hi) in enumerate(batches):
        count = hi - lo
        for k in range(max(lo, 1), hi):
            pick_copy(k).wait_recv()
            relay_copy(k).start()
        y0, y1 = None, None
        for s, base in ((0, h), (1, partner)):
            if s == 1:
                for k in range(lo, hi):
                    relay_copy(k).wait_recv()
            x0 = arrived[s, lo:hi, :pad].reshape(count * pad, side)
            x1 = arrived[s, lo:hi, full:].reshape(count * pad, side)
            p0 = dot(x0, gu_w[pl.ds(pl.multiple_of(base * half, side), side), :])
            p1 = dot(x1, gu_w[pl.ds(pl.multiple_of(base * half + side, side), side), :])
            y0, y1 = (p0, p1) if s == 0 else (y0 + p0, y1 + p1)
        y = merge(y0.reshape(count, pad, 2 * ff), y1.reshape(count, pad, 2 * ff), full).reshape(count * pad, 2 * ff)
        g = y[:, :ff]
        span = slice(lo * pad, hi * pad)
        hid_own[span] = (g / (1.0 + jnp.exp(-g)) * y[:, ff:]).astype(bf16)
        hid_copy(i).start()
        if i == 0:
            load_down.wait()
        part = dot(hid_own[span], down_own[...])
        if i == 0:
            send_down.wait_recv()
        hid_copy(i).wait_recv()
        part = part + dot(hid_other[span], down_other[...])
        outs[lo:hi] = pack(part.reshape(count, pad, half), full)
        for k in range(max(lo, 1), hi):
            ret_copy(k).start()
        if lo == 0:
            keep = pltpu.make_async_copy(outs.at[0], ret.at[0], load_sem.at[7])
            keep.start()

    for i, (lo, hi) in enumerate(batches):
        for k in range(max(lo, 1), hi):
            ret_copy(k).wait_recv()
    keep.wait()
    put.wait()
    send_down.wait_send()
    for i in range(len(batches)):
        hid_copy(i).wait_send()
    for k in range(n):
        relay_copy(k).wait_send()
        if k:
            pick_copy(k).wait_send()
            ret_copy(k).wait_send()


def combine_kernel(full, ret_hbm, factors_hbm, out_hbm, ret, factors, out, sem):
    side = ret.shape[2]
    total = factors.shape[2]
    pad = full + 8
    take = [
        pltpu.make_async_copy(factors_hbm, factors, sem.at[0]),
        pltpu.make_async_copy(ret_hbm.at[:, :pad], ret.at[:, :pad], sem.at[1]),
        pltpu.make_async_copy(ret_hbm.at[:, pad:], ret.at[:, pad:], sem.at[2]),
    ]
    put = [pltpu.make_async_copy(out.at[i], out_hbm.at[:, i * side:(i + 1) * side], sem.at[3 + i]) for i in range(2)]
    for copy in take:
        copy.start()
    take[0].wait()
    take[1].wait()
    out[0] = dot(factors[0], ret[:, :pad].reshape(total, side)).astype(bf16)
    put[0].start()
    take[2].wait()
    out[1] = dot(factors[1], ret[:, full:].reshape(total, side)).astype(bf16)
    put[1].start()
    put[0].wait()
    put[1].wait()


def solution(mesh):
    n = mesh.shape["ep"]

    def shards(tokens, norm_gain, gate_weight, up_weight, down_weight, chosen, affinity):
        rows, width = tokens.shape
        ff = gate_weight.shape[2]
        slot = chosen.shape[2]
        full = slot // 8 * 8 if 0 < slot % 8 <= 4 else -(-slot // 8) * 8
        pad = full + 8
        half = width // 2
        message = (n, 2 * full + 8, half // 2)
        any_spec = pl.BlockSpec(memory_space=pl.ANY)
        dma = pltpu.SemaphoreType.DMA
        factors = jax.ShapeDtypeStruct((2, rows, n * pad), bf16)
        ret, factors = pl.pallas_call(
            functools.partial(kernel, n, full),
            out_shape=(jax.ShapeDtypeStruct(message, bf16), factors),
            in_specs=[any_spec] * 7,
            out_specs=(any_spec, any_spec),
            scratch_shapes=[
                pltpu.VMEM((2, rows, n * pad), bf16),
                pltpu.VMEM((rows, width), bf16),
                pltpu.VMEM((1, width), f32),
                pltpu.VMEM(chosen.shape[1:], jnp.int32),
                pltpu.VMEM(affinity.shape[1:], f32),
                pltpu.VMEM((width, 2 * ff), bf16),
                pltpu.VMEM((ff, half), bf16),
                pltpu.VMEM((ff, half), bf16),
                pltpu.VMEM((rows, half), bf16),
                pltpu.VMEM(message, bf16),
                pltpu.VMEM((2,) + message, bf16),
                pltpu.VMEM((n * pad, ff), bf16),
                pltpu.VMEM((n * pad, ff), bf16),
                pltpu.VMEM(message, bf16),
                dma((9,)),
                dma((2,)),
                dma((n,)),
                dma((n,)),
                dma((n,)),
                dma((n,)),
                dma((3,)),
                dma((3,)),
                dma((n,)),
                dma((n,)),
            ],
            compiler_params=pltpu.CompilerParams(
                collective_id=0, has_side_effects=True, vmem_limit_bytes=56 * 1024 * 1024
            ),
        )(tokens, norm_gain.reshape(1, -1), gate_weight, up_weight, down_weight, chosen[0], affinity[0])
        return pl.pallas_call(
            functools.partial(combine_kernel, full),
            out_shape=jax.ShapeDtypeStruct((rows, half), bf16),
            in_specs=[any_spec] * 2,
            out_specs=any_spec,
            scratch_shapes=[
                pltpu.VMEM(message, bf16),
                pltpu.VMEM((2, rows, n * pad), bf16),
                pltpu.VMEM((2, rows, half // 2), bf16),
                dma((5,)),
            ],
            compiler_params=pltpu.CompilerParams(vmem_limit_bytes=56 * 1024 * 1024),
        )(ret, factors)

    in_specs = (
        P(("grp", "ep"), None),
        P(),
        P("ep", None, "tp"),
        P("ep", None, "tp"),
        P("ep", "tp", None),
        P(("grp", "ep"), None, None),
        P(("grp", "ep"), None, None),
    )
    out_specs = P(("grp", "ep"), "tp")
    return jax.shard_map(shards, mesh=mesh, in_specs=in_specs, out_specs=out_specs, check_vma=False)
```

```python
import functools

import jax
import jax.numpy as jnp
from jax import lax
from jax.experimental import pallas as pl
from jax.experimental.pallas import tpu as pltpu
from jax.sharding import PartitionSpec as P

norm_eps = 1e-06
bf16, f32 = jnp.bfloat16, jnp.float32


def dot(a, b):
    return jnp.dot(a, b, preferred_element_type=f32)


def iota(shape, dim):
    return lax.broadcasted_iota(jnp.int32, shape, dim)


def merge(y0, y1, full):
    return jnp.concatenate(
        [y0[:, :full] + y1[:, 8:], y0[:, full:] + pltpu.roll(y1[:, :8], 4, 1)], axis=1)


def pack(y, full):
    side = y.shape[2] // 2
    y0, y1 = y[:, :, :side], y[:, :, side:]
    upper = iota((y.shape[0], 8, side), 1) < 4
    rest = jnp.where(upper, y0[:, full:], pltpu.roll(y1[:, full:], 4, 1))
    return jnp.concatenate([y0[:, :full], rest, y1[:, :full]], axis=1).astype(bf16)


def kernel(n, full, tok_hbm, gain_hbm, gate_hbm, up_hbm, down_hbm, chosen_hbm, aff_hbm, ret, factors_hbm,
           factors, tok, gain_ref, chosen_ref, aff_ref, gu_w, down_own, down_other, normed, picks, arrived, hid_own, hid_other, outs,
           load_sem, wd_sem, pick_send, pick_recv, relay_send, relay_recv, hid_send, hid_recv, ret_send, ret_recv):
    me = lax.axis_index("ep")
    h = lax.axis_index("tp")
    partner = 1 - h
    rows, width = tok.shape
    half = width // 2
    side = half // 2
    ff = down_own.shape[0]
    slot = chosen_ref.shape[1]
    pad = full + 8
    total = n * pad
    paired = n & (n - 1) == 0
    mesh_id = pl.DeviceIdType.MESH

    def to(k):
        return me ^ k if paired else lax.rem(me + k, n)

    def back(k):
        return me ^ k if paired else lax.rem(me + n - k, n)

    place_k = (lambda e: e ^ me) if paired else (lambda e: lax.rem(e + n - me, n))
    if n >= 4:
        batches = [(0, n // 2), (n // 2, n // 2 + n // 4), (n // 2 + n // 4, n)]
        order = list(range(n // 2, n)) + list(range(1, n // 2))
    else:
        batches = [(0, n)]
        order = list(range(1, n))

    load_tok = pltpu.make_async_copy(tok_hbm, tok, load_sem.at[0])
    load_tok.start()
    load_gain = pltpu.make_async_copy(gain_hbm, gain_ref, load_sem.at[4])
    load_gain.start()
    load_chosen = pltpu.make_async_copy(chosen_hbm, chosen_ref, load_sem.at[5])
    load_chosen.start()
    load_aff = pltpu.make_async_copy(aff_hbm, aff_ref, load_sem.at[6])
    load_aff.start()

    barrier = pltpu.get_barrier_semaphore()
    for k in order:
        pl.semaphore_signal(barrier, inc=1, device_id={"ep": to(k)}, device_id_type=mesh_id)
    pl.semaphore_signal(barrier, inc=1, device_id={"tp": partner}, device_id_type=mesh_id)

    my_cols = pl.multiple_of(h * half, half)
    partner_cols = pl.multiple_of(partner * half, half)
    load_gate = pltpu.make_async_copy(gate_hbm.at[0], gu_w.at[:, :ff], load_sem.at[1])
    load_up = pltpu.make_async_copy(up_hbm.at[0], gu_w.at[:, ff:], load_sem.at[2])
    load_down = pltpu.make_async_copy(down_hbm.at[0, :, pl.ds(my_cols, half)], down_own, load_sem.at[3])
    load_gate.start()
    load_up.start()
    load_down.start()

    load_chosen.wait()
    picked = chosen_ref[...].astype(f32).astype(bf16)
    row = iota((total, n), 0)
    first = place_k(iota((total, n), 1)) * pad
    spread = jnp.where((row >= first) & (row < first + pad), 1.0, 0.0).astype(bf16)
    wide = dot(spread, picked)
    within = lax.rem(iota((total, slot), 0), pad) == iota((total, slot), 1)
    column = jnp.sum(jnp.where(within, wide + 1.0, 0.0), axis=1, keepdims=True) - 1.0
    select = jnp.where(iota((total, rows), 1).astype(f32) == column, 1.0, 0.0).astype(bf16)

    load_tok.wait()
    load_gain.wait()
    squares = jnp.zeros((rows, 1), f32)
    for i in range(8):
        piece = tok[:, i * (width // 8):(i + 1) * (width // 8)].astype(f32)
        squares = squares + jnp.sum(piece * piece, axis=1, keepdims=True)
    scale = lax.rsqrt(squares / width + norm_eps)
    for i in range(4):
        cols = pl.ds(pl.multiple_of(h * half + i * (half // 4), half // 4), half // 4)
        normed[:, i * (half // 4):(i + 1) * (half // 4)] = (
            tok[:, cols].astype(f32) * scale * gain_ref[:, cols]).astype(bf16)

    def pick_copy(k):
        return pltpu.make_async_remote_copy(
            picks.at[k], arrived.at[0, k], pick_send.at[k], pick_recv.at[k],
            device_id={"ep": to(k)}, device_id_type=mesh_id)

    def relay_copy(k):
        source = picks.at[0] if k == 0 else arrived.at[0, k]
        return pltpu.make_async_remote_copy(
            source, arrived.at[1, k], relay_send.at[k], relay_recv.at[k],
            device_id={"tp": partner}, device_id_type=mesh_id)

    def hid_copy(i):
        span = pl.ds(batches[i][0] * pad, (batches[i][1] - batches[i][0]) * pad)
        return pltpu.make_async_remote_copy(
            hid_own.at[span], hid_other.at[span], hid_send.at[i], hid_recv.at[i],
            device_id={"tp": partner}, device_id_type=mesh_id)

    def ret_copy(k):
        return pltpu.make_async_remote_copy(
            outs.at[k], ret.at[k], ret_send.at[k], ret_recv.at[k],
            device_id={"ep": back(k)}, device_id_type=mesh_id)

    for i, (lo, hi) in enumerate([(0, n // 2), (n // 2, n // 2 + n // 4), (n // 2 + n // 4, n)]):
        taken = dot(select[lo * pad:hi * pad], normed[...])
        picks[lo:hi] = pack(taken.reshape(hi - lo, pad, half), full)
        if i == 0:
            pl.semaphore_wait(barrier, n)
        for k in (range(1, hi) if lo == 0 else range(hi - 1, lo - 1, -1)):
            pick_copy(k).start()
    arrived[0, 0] = picks[0]
    relay_copy(0).start()

    send_down = pltpu.make_async_remote_copy(
        down_hbm.at[0, :, pl.ds(partner_cols, half)], down_other, wd_sem.at[0], wd_sem.at[1],
        device_id={"tp": partner}, device_id_type=mesh_id)
    send_down.start()

    slot_low = place_k(iota((n, total), 0)) * pad
    lane = iota((n, total), 1)
    mine = (lane >= slot_low) & (lane < slot_low + pad)
    load_aff.wait()
    weights = aff_ref[...].astype(bf16)

    def combine_of(second):
        at = lax.rem(iota((slot, total), 1), pad)
        if second:
            at = jnp.where(at < 4, -1, jnp.where(at < 8, at + (full - 4), at - 8))
        place = jnp.where(at == iota((slot, total), 0), 1.0, 0.0).astype(bf16)
        row_of = jnp.sum(jnp.where(mine, dot(picked, place), 0.0), axis=0, keepdims=True)
        filled = jnp.sum(place.astype(f32), axis=0, keepdims=True)
        row_of = jnp.where(filled > 0.5, row_of, -1.0)
        value = jnp.sum(jnp.where(mine, dot(weights, place), 0.0), axis=0, keepdims=True)
        return jnp.where(iota((rows, total), 0).astype(f32) == row_of, value, 0.0).astype(bf16)

    factors[0] = combine_of(False)
    factors[1] = combine_of(True)
    put = pltpu.make_async_copy(factors, factors_hbm, load_sem.at[8])
    put.start()

    load_gate.wait()
    load_up.wait()
    for i, (lo, hi) in enumerate(batches):
        count = hi - lo
        for k in range(max(lo, 1), hi):
            pick_copy(k).wait_recv()
            relay_copy(k).start()
        y0, y1 = None, None
        for s, base in ((0, h), (1, partner)):
            if s == 1:
                for k in range(lo, hi):
                    relay_copy(k).wait_recv()
            x0 = arrived[s, lo:hi, :pad].reshape(count * pad, side)
            x1 = arrived[s, lo:hi, full:].reshape(count * pad, side)
            p0 = dot(x0, gu_w[pl.ds(pl.multiple_of(base * half, side), side), :])
            p1 = dot(x1, gu_w[pl.ds(pl.multiple_of(base * half + side, side), side), :])
            y0, y1 = (p0, p1) if s == 0 else (y0 + p0, y1 + p1)
        y = merge(y0.reshape(count, pad, 2 * ff), y1.reshape(count, pad, 2 * ff), full).reshape(count * pad, 2 * ff)
        g = y[:, :ff]
        span = slice(lo * pad, hi * pad)
        hid_own[span] = (g / (1.0 + jnp.exp(-g)) * y[:, ff:]).astype(bf16)
        hid_copy(i).start()
        if i == 0:
            load_down.wait()
        part = dot(hid_own[span], down_own[...])
        if i == 0:
            send_down.wait_recv()
        hid_copy(i).wait_recv()
        part = part + dot(hid_other[span], down_other[...])
        outs[lo:hi] = pack(part.reshape(count, pad, half), full)
        for k in range(hi - 1, max(lo, 1) - 1, -1):
            ret_copy(k).start()
        if lo == 0:
            keep = pltpu.make_async_copy(outs.at[0], ret.at[0], load_sem.at[7])
            keep.start()

    for i, (lo, hi) in enumerate(batches):
        for k in range(max(lo, 1), hi):
            ret_copy(k).wait_recv()
    keep.wait()
    put.wait()
    send_down.wait_send()
    for i in range(len(batches)):
        hid_copy(i).wait_send()
    for k in range(n):
        relay_copy(k).wait_send()
        if k:
            pick_copy(k).wait_send()
            ret_copy(k).wait_send()


def combine_kernel(full, ret_hbm, factors_hbm, out_hbm, ret, factors, out, sem):
    side = ret.shape[2]
    total = factors.shape[2]
    pad = full + 8
    take = [
        pltpu.make_async_copy(factors_hbm, factors, sem.at[0]),
        pltpu.make_async_copy(ret_hbm.at[:, :pad], ret.at[:, :pad], sem.at[1]),
        pltpu.make_async_copy(ret_hbm.at[:, pad:], ret.at[:, pad:], sem.at[2]),
    ]
    put = [pltpu.make_async_copy(out.at[i], out_hbm.at[:, i * side:(i + 1) * side], sem.at[3 + i]) for i in range(2)]
    for copy in take:
        copy.start()
    take[0].wait()
    take[1].wait()
    out[0] = dot(factors[0], ret[:, :pad].reshape(total, side)).astype(bf16)
    put[0].start()
    take[2].wait()
    out[1] = dot(factors[1], ret[:, full:].reshape(total, side)).astype(bf16)
    put[1].start()
    put[0].wait()
    put[1].wait()


def solution(mesh):
    n = mesh.shape["ep"]

    def shards(tokens, norm_gain, gate_weight, up_weight, down_weight, chosen, affinity):
        rows, width = tokens.shape
        ff = gate_weight.shape[2]
        slot = chosen.shape[2]
        full = slot // 8 * 8 if 0 < slot % 8 <= 4 else -(-slot // 8) * 8
        pad = full + 8
        half = width // 2
        message = (n, 2 * full + 8, half // 2)
        any_spec = pl.BlockSpec(memory_space=pl.ANY)
        dma = pltpu.SemaphoreType.DMA
        factors = jax.ShapeDtypeStruct((2, rows, n * pad), bf16)
        ret, factors = pl.pallas_call(
            functools.partial(kernel, n, full),
            out_shape=(jax.ShapeDtypeStruct(message, bf16), factors),
            in_specs=[any_spec] * 7,
            out_specs=(any_spec, any_spec),
            scratch_shapes=[
                pltpu.VMEM((2, rows, n * pad), bf16),
                pltpu.VMEM((rows, width), bf16),
                pltpu.VMEM((1, width), f32),
                pltpu.VMEM(chosen.shape[1:], jnp.int32),
                pltpu.VMEM(affinity.shape[1:], f32),
                pltpu.VMEM((width, 2 * ff), bf16),
                pltpu.VMEM((ff, half), bf16),
                pltpu.VMEM((ff, half), bf16),
                pltpu.VMEM((rows, half), bf16),
                pltpu.VMEM(message, bf16),
                pltpu.VMEM((2,) + message, bf16),
                pltpu.VMEM((n * pad, ff), bf16),
                pltpu.VMEM((n * pad, ff), bf16),
                pltpu.VMEM(message, bf16),
                dma((9,)),
                dma((2,)),
                dma((n,)),
                dma((n,)),
                dma((n,)),
                dma((n,)),
                dma((3,)),
                dma((3,)),
                dma((n,)),
                dma((n,)),
            ],
            compiler_params=pltpu.CompilerParams(
                collective_id=0, has_side_effects=True, vmem_limit_bytes=56 * 1024 * 1024
            ),
        )(tokens, norm_gain.reshape(1, -1), gate_weight, up_weight, down_weight, chosen[0], affinity[0])
        return pl.pallas_call(
            functools.partial(combine_kernel, full),
            out_shape=jax.ShapeDtypeStruct((rows, half), bf16),
            in_specs=[any_spec] * 2,
            out_specs=any_spec,
            scratch_shapes=[
                pltpu.VMEM(message, bf16),
                pltpu.VMEM((2, rows, n * pad), bf16),
                pltpu.VMEM((2, rows, half // 2), bf16),
                dma((5,)),
            ],
            compiler_params=pltpu.CompilerParams(vmem_limit_bytes=56 * 1024 * 1024),
        )(ret, factors)

    in_specs = (
        P(("grp", "ep"), None),
        P(),
        P("ep", None, "tp"),
        P("ep", None, "tp"),
        P("ep", "tp", None),
        P(("grp", "ep"), None, None),
        P(("grp", "ep"), None, None),
    )
    out_specs = P(("grp", "ep"), "tp")
    return jax.shard_map(shards, mesh=mesh, in_specs=in_specs, out_specs=out_specs, check_vma=False)
```
